32 devices in a mesh: sp: 8 (over z, x), tp: 4 (over y, core).
Axes of the slice: x: 2, y: 2, z: 4, core: 2. Of those that a mesh axis runs over, the one named last changes fastest.
Arguments:
- stream_in: bfloat16 [2048, 2048], P(('sp', 'tp')), may hold values from -6 to 6
- pre_gate: bfloat16 [2048, 1024], P('sp', 'tp'), may hold values from -6 to 6
- value_in: bfloat16 [2048, 1024], P('sp', 'tp'), may hold values from -6 to 6
- post_gate: bfloat16 [2048, 1024], P('sp', 'tp'), may hold values from -6 to 6
- conv_taps: bfloat16 [3, 1024], P(None, 'tp'), may hold values from -3 to 3
- out_weight: bfloat16 [1024, 2048], P('tp'), may hold values from -0.1875 to 0.1875
- route_ids: int32 [2048, 4], P('sp'), may hold values from 0 to 7, all different within a row; in each aligned block of 64 rows (0 to 63, 64 to 127, ...) at most 64 rows name the same one
- route_weight: float32 [2048, 4], P('sp'), may hold values from 0.1 to 1
- ffn_gain: bfloat16 [2048], replicated, may hold values from 0.099609375 to 1.8984375
- post_gain: bfloat16 [2048], replicated, may hold values from 0.099609375 to 1.8984375
- gate_proj: bfloat16 [8, 2048, 2048], P('sp', None, 'tp'), may hold values from -0.39648438 to 0.39648438
- up_proj: bfloat16 [8, 2048, 2048], P('sp', None, 'tp'), may hold values from -0.39648438 to 0.39648438
- down_proj: bfloat16 [8, 2048, 2048], P('sp', None, 'tp'), may hold values from -0.125 to 0.125
Outputs:
- layer_out: bfloat16 [2048, 2048], P(('sp', 'tp'))
The draws below stay inside these ranges and needn't reach their ends.
Inputs may be any that keep to these rules, and one draw needn't show every extreme that they name: `route_ids`: in each aligned block of 64 positions, a row names 4 different experts and no expert is named by more than 64 rows; in every draw some expert reaches 64 in some block.
All inputs are finite; a program needn't handle non-finite values.
Results may differ from the reference program's by a relative error of at most 0.014.
Values may be sent and summed in bfloat16 or wider, within the bound.
A program may use at most 64 MiB of HBM per device.

```python
import math
import jax
import jax.numpy as jnp
import numpy as np
from jax import lax

D = 2048
W = 1024
FF = 2048
TOPK = 4
KERNEL = 3
TOKENS = 2048
EXPERTS = 8
ROWS = 64
CAP = 64
SLOTS = 2048


def shard_levels(key, extent, shards, low, top_value):
    level, own = 1.0, jax.random.fold_in(key, 6)
    for position, blocks in shards:
        heights = jnp.exp(jax.random.uniform(jax.random.fold_in(own, position), (blocks,), jnp.float32, low / len(shards), top_value / len(shards)))
        level = level * jnp.repeat(heights, extent[position] // blocks).reshape([-1 if axis == position else 1 for axis in range(len(extent))])
    return level


def deal_out(stream_key, own, number, rows, count, top, bound, slope):
    sequence = jax.random.permutation(stream_key, count)
    crowded, ordinary = load_shares(count, rows * top, bound, slope, True), load_shares(count, rows * top, bound, slope, False)
    places = jnp.arange(count)

    def named(lengths, rotation):
        used = int((lengths > 0).sum())
        fixed = max(1, used // 4)
        moved = fixed + (places - fixed + rotation * (used - fixed)) % max(1, count - fixed)
        return jnp.zeros((count,), jnp.int32).at[sequence[jnp.where(places < fixed, places, moved)]].set(jnp.asarray(lengths, jnp.int32))

    lengths = jnp.where(number % 4 == 0, named(crowded, number // 4), named(ordinary, number - number // 4 - 1))
    mixed = jax.random.permutation(jax.random.fold_in(own, 3), count)
    donor, receiver = mixed[0:count // 2 * 2:2], mixed[1:count // 2 * 2:2]
    margin = jnp.minimum(lengths[donor] - 1, bound - lengths[receiver]) // 2
    margin = jnp.where((donor == sequence[0]) | (receiver == sequence[0]) | (lengths[receiver] == 0), 0, jnp.maximum(margin, 0))
    moved = jax.random.randint(jax.random.fold_in(own, 4), (count // 2,), 0, 1 << 20) % (margin + 1)
    lengths = lengths.at[donor].add(-moved).at[receiver].add(moved)
    members = jnp.searchsorted(jnp.cumsum(lengths), jnp.arange(rows * top), side="right").astype(jnp.int32)
    grid = members.reshape(top, rows).T
    grid = grid[jax.random.permutation(jax.random.fold_in(own, 1), rows)]
    rotation = jax.random.randint(jax.random.fold_in(own, 2), (rows, 1), 0, top)
    return jnp.take_along_axis(grid, (jnp.arange(top)[None, :] + rotation) % top, axis=1)


def load_shares(number_of, total, bound, lean, full):
    portions = [(1 << 20) // math.isqrt(standing ** lean) + 1 for standing in range(1, number_of + 1)]
    largest = bound if full else min(bound, max(-(-total // number_of), total * portions[0] // sum(portions)))
    least = 1 if total - largest >= number_of - 1 else 0
    counts, rest = [largest] + [least] * (number_of - 1), total - largest - least * (number_of - 1)
    while rest > 0:
        candidates = [i for i in range(1, number_of) if counts[i] < largest] or [i for i in range(1, number_of) if counts[i] < bound]
        whole, remaining = sum([portions[i] for i in candidates]), rest
        for i in candidates:
            addition = min(bound - counts[i], max(1, remaining * portions[i] // whole), rest)
            counts[i] = counts[i] + addition
            rest = rest - addition
    return np.array(counts)


def normal_values(rng, extent, width, limit, split=(), kind=jnp.bfloat16):
    drawn = width * jax.random.normal(rng, extent, jnp.float32)
    if split:
        drawn = drawn * shard_levels(rng, extent, split, -0.22, 0.18)
    return jnp.clip(drawn, -limit, limit).astype(kind)


def setup_inputs(seed: int = 0) -> dict:
    key_of = jax.random.split(jax.random.key(seed), 14)
    stream_in = normal_values(key_of[0], (TOKENS, D), 1.0, 6.0, ((0, 32),))
    pre_gate = normal_values(key_of[1], (TOKENS, W), 1.0, 6.0, ((0, 8), (1, 4)))
    value_in = normal_values(key_of[2], (TOKENS, W), 1.0, 6.0, ((0, 8), (1, 4)))
    post_gate = normal_values(key_of[3], (TOKENS, W), 1.0, 6.0, ((0, 8), (1, 4)))
    conv_taps = normal_values(key_of[4], (KERNEL, W), 0.6, 3.0, ((1, 4),))
    out_weight = normal_values(key_of[5], (W, D), W ** -0.5, 0.1875, ((0, 4),))
    route_ids_keys = jax.random.split(jax.random.fold_in(key_of[6], 1), TOKENS // ROWS)
    route_ids_turns = jax.random.permutation(jax.random.fold_in(key_of[6], 3), TOKENS // ROWS)
    route_ids = jax.vmap(lambda own, number: deal_out(jax.random.fold_in(key_of[6], 2), own, number, ROWS, EXPERTS, TOPK, CAP, 2))(route_ids_keys, route_ids_turns).reshape((TOKENS, TOPK))
    route_weight = jnp.clip(jnp.exp(math.log(1.0) - 2.3025851 * jax.random.uniform(key_of[7], (TOKENS, TOPK), jnp.float32) ** shard_levels(key_of[7], (TOKENS, TOPK), ((0, 8),), -0.2, 0.2)), 0.1, 1.0)
    ffn_gain = jnp.clip(1.0 + 0.18 * jax.random.normal(key_of[8], (D,), jnp.float32), 0.099609375, 1.8984375).astype(jnp.bfloat16)
    post_gain = jnp.clip(1.0 + 0.18 * jax.random.normal(key_of[9], (D,), jnp.float32), 0.099609375, 1.8984375).astype(jnp.bfloat16)
    gate_proj = normal_values(key_of[10], (EXPERTS, D, FF), (3.0 * D ** -0.5), 0.39648438, ((0, 8), (2, 4)))
    up_proj = normal_values(key_of[11], (EXPERTS, D, FF), (3.0 * D ** -0.5), 0.39648438, ((0, 8), (2, 4)))
    down_proj = normal_values(key_of[12], (EXPERTS, FF, D), FF ** -0.5, 0.125, ((0, 8), (2, 4)))
    return dict(stream_in=stream_in, pre_gate=pre_gate, value_in=value_in, post_gate=post_gate, conv_taps=conv_taps, out_weight=out_weight, route_ids=route_ids, route_weight=route_weight, ffn_gain=ffn_gain, post_gain=post_gain, gate_proj=gate_proj, up_proj=up_proj, down_proj=down_proj)


clamp_limit = 7.0
sigmoid_scale = 1.702
epsilon = 1e-06

def clamped_units(gate_pre, up_pre):
    gate_cut = jnp.minimum(gate_pre, clamp_limit)
    up_cut = jnp.clip(up_pre, -clamp_limit, clamp_limit)
    return (up_cut + 1.0) * (gate_cut * jax.nn.sigmoid(sigmoid_scale * gate_cut))

def scaled_norm(values, gain):
    return values * lax.rsqrt(lax.optimization_barrier(jnp.mean(values * values, axis=-1, keepdims=True)) + epsilon) * gain.astype(jnp.float32)

def reference(stream_in, pre_gate, value_in, post_gate, conv_taps, out_weight, route_ids, route_weight, ffn_gain, post_gain, gate_proj, up_proj, down_proj):
    tap_count = conv_taps.shape[0]
    gated_input = (pre_gate.astype(jnp.float32) * value_in.astype(jnp.float32)).astype(jnp.bfloat16)
    padded = jnp.concatenate([jnp.zeros((tap_count - 1, W), jnp.bfloat16), gated_input], 0).astype(jnp.float32)
    convolved = jnp.zeros((TOKENS, W), jnp.float32)
    for tap_index in range(tap_count):
        convolved = convolved + conv_taps[tap_index].astype(jnp.float32)[None, :] * padded[tap_index:tap_index + TOKENS]
    mixer_out = (post_gate.astype(jnp.float32) * convolved).astype(jnp.bfloat16)
    projected = jnp.dot(mixer_out, out_weight, preferred_element_type=jnp.float32)
    residual = (stream_in.astype(jnp.float32) + projected).astype(jnp.bfloat16)
    normed = scaled_norm(residual.astype(jnp.float32), ffn_gain).astype(jnp.bfloat16)
    flattened = route_ids.reshape(-1).astype(jnp.int32)
    entries = flattened.shape[0]
    onehot = (flattened[:, None] == jnp.arange(EXPERTS, dtype=jnp.int32)[None, :]).astype(jnp.int32)
    blocked = onehot.reshape(entries // (ROWS * TOPK), ROWS * TOPK, EXPERTS)
    before = jnp.cumsum(blocked, axis=1) - blocked
    slot_rank = lax.optimization_barrier(jnp.sum(before * blocked, axis=2)).reshape(entries)
    block_ids = jnp.arange(entries, dtype=jnp.int32) // (ROWS * TOPK)
    slot_index = (block_ids * CAP + slot_rank).astype(jnp.int32)
    token_ids = jnp.arange(entries, dtype=jnp.int32) // TOPK
    slot_table = jnp.full((EXPERTS, SLOTS), TOKENS, jnp.int32).at[flattened, slot_index].set(token_ids)
    padded_rows = jnp.concatenate([normed, jnp.zeros((1, D), jnp.bfloat16)], 0)

    def one_expert(packed):
        token_rows, gate_matrix, up_matrix, down_matrix = packed
        inputs = padded_rows[token_rows]
        gate_pre = jnp.dot(inputs, gate_matrix, preferred_element_type=jnp.float32)
        up_pre = jnp.dot(inputs, up_matrix, preferred_element_type=jnp.float32)
        hidden = clamped_units(gate_pre, up_pre).astype(jnp.bfloat16)
        return jnp.dot(hidden, down_matrix, preferred_element_type=jnp.float32).astype(jnp.bfloat16)
    expert_outs = lax.map(one_expert, (slot_table, gate_proj, up_proj, down_proj))
    picked = expert_outs[flattened, slot_index].astype(jnp.float32).reshape(TOKENS, TOPK, D)
    combined = lax.optimization_barrier(jnp.sum(picked * route_weight[:, :, None], axis=1)).astype(jnp.bfloat16)
    layer_out = residual.astype(jnp.float32) + scaled_norm(combined.astype(jnp.float32), post_gain)
    return layer_out.astype(jnp.bfloat16)
```

```python
import functools

import jax
import jax.numpy as jnp
from jax import lax
from jax.experimental import pallas as pl
from jax.experimental.pallas import tpu as pltpu
from jax.sharding import PartitionSpec as P

clamp_limit = 7.0
sigmoid_scale = 1.702
epsilon = 1e-06


def passed_along(array, axis, by):
    count = lax.axis_size(axis)
    pairs = [(i, i + by) for i in range(count) if 0 <= i + by < count]
    return lax.ppermute(array, axis, pairs)


def clamped_units(gate_pre, up_pre):
    gate_cut = jnp.minimum(gate_pre, clamp_limit)
    up_cut = jnp.clip(up_pre, -clamp_limit, clamp_limit)
    return (up_cut + 1.0) * (gate_cut * jax.nn.sigmoid(sigmoid_scale * gate_cut))


def scaled_norm(values, gain):
    return (
        values
        * lax.rsqrt(jnp.mean(values * values, axis=-1, keepdims=True) + epsilon)
        * gain.astype(jnp.float32)
    )


def block_ranks(route_rows, experts, block_rows):
    flattened = route_rows.reshape(-1)
    entries = flattened.shape[0]
    span_width = block_rows * route_rows.shape[1]
    onehot = (flattened[:, None] == jnp.arange(experts, dtype=jnp.int32)[None, :]).astype(jnp.int32)
    blocked = onehot.reshape(entries // span_width, span_width, experts)
    before = jnp.cumsum(blocked, axis=1) - blocked
    return jnp.sum(before * blocked, axis=2).reshape(route_rows.shape)


def slot_picker(slot_index, table_size):
    matches = slot_index[None, :, :] == jnp.arange(table_size, dtype=jnp.int32)[:, None, None]
    return jnp.any(matches, axis=2).astype(jnp.bfloat16)


LANES = 128


def table_pick(table, first, second):
    value = jnp.int32(0)
    for i, row in enumerate(table):
        for j, entry in enumerate(row):
            if entry:
                value = value + jnp.where((first == i) & (second == j), entry, 0)
    return value


def layer_kernel(
    sp_count,
    stream_ref,
    pre_ref,
    value_ref,
    post_ref,
    taps_ref,
    ids_ref,
    weight_ref,
    gain_ref,
    post_gain_ref,
    out_hbm,
    gate_hbm,
    up_hbm,
    down_hbm,
    result_ref,
    out_w,
    gate_w,
    up_w,
    down_w,
    tail,
    rim,
    padded,
    mixed,
    pair_send,
    pair_in,
    own_sum,
    y_send,
    y_in,
    resid,
    tokens,
    hidden,
    part,
    chain_in,
    x_in,
    final,
    columns,
    load_sem,
    rim_sem,
    proj_sem,
    y_sem,
    tok_send,
    tok_recv,
    hid_send,
    hid_recv,
    chain_send,
    chain_recv,
    x_sem,
    fin_send,
    fin_recv,
):
    f32, bf16 = jnp.float32, jnp.bfloat16
    heights = sp_count // 2
    sp = lax.axis_index("sp")
    tp = lax.axis_index("tp")
    z, x = lax.div(sp, 2), lax.rem(sp, 2)
    y, c = lax.div(tp, 2), lax.rem(tp, 2)
    across, sibling = sp + 1 - 2 * x, tp + 1 - 2 * c
    opposite = lax.rem(tp + 2, 4)
    rows, width = stream_ref.shape
    seq = 4 * rows
    half = 2 * rows
    units = gate_w.shape[1]

    def at(sp_to, tp_to):
        return {"sp": sp_to, "tp": tp_to}

    def remote(source, target, send, receive, device):
        return pltpu.make_async_remote_copy(
            src_ref=source,
            dst_ref=target,
            send_sem=send,
            recv_sem=receive,
            device_id=device,
            device_id_type=pl.DeviceIdType.MESH,
        )

    loads = [
        pltpu.make_async_copy(source, target, load_sem.at[i])
        for i, (source, target) in enumerate(
            ((out_hbm, out_w), (gate_hbm.at[0], gate_w), (up_hbm.at[0], up_w), (down_hbm.at[0], down_w))
        )
    ]
    for load in loads:
        load.start()

    barrier = pltpu.get_barrier_semaphore()
    partners = [at(lax.rem(sp + by, sp_count), tp) for by in (1, 2, sp_count - 1, sp_count - 2)]
    partners += [at(across, tp), at(sp, sibling), at(sp, opposite), at(sp, 3 - tp)]
    for partner in partners:
        pl.semaphore_signal(barrier, inc=1, device_id=partner, device_id_type=pl.DeviceIdType.MESH)
    pl.semaphore_wait(barrier, len(partners))

    gated = (pre_ref[...].astype(f32) * value_ref[...].astype(f32)).astype(bf16)
    tail[...] = gated[seq - 16 :]
    rim_copy = remote(tail, rim, rim_sem.at[0], rim_sem.at[1], at(lax.rem(sp + 1, sp_count), tp))
    rim_copy.start()
    padded[8:, :] = gated.astype(f32)
    lane = lax.broadcasted_iota(jnp.int32, (rows, LANES), 1)
    ids = ids_ref[pl.ds(pl.multiple_of(tp * rows, rows), rows), :]
    weights = weight_ref[pl.ds(pl.multiple_of(tp * rows, rows), rows), :]
    spread = jnp.zeros((rows, LANES), f32)
    for k in range(ids.shape[1]):
        one = weights[:, k : k + 1]
        high = one.astype(bf16).astype(f32)
        spread = spread + jnp.where(lane == ids[:, k : k + 1], high, 0.0)
        spread = spread + jnp.where(lane == ids[:, k : k + 1] + sp_count, one - high, 0.0)
    own_row = pl.multiple_of(c * half + y * rows, rows)
    tokens[sp, pl.ds(own_row, rows), width:] = spread.astype(bf16)
    rim_copy.wait()
    padded[:8, :] = jnp.where(sp == 0, 0.0, rim[...].astype(f32)[8:])
    tap_count = taps_ref.shape[0]
    taps = taps_ref[...].astype(f32)
    convolved = jnp.zeros((seq, padded.shape[1]), f32)
    for k in range(tap_count):
        first = 8 - tap_count + 1 + k
        convolved = convolved + taps[k : k + 1, :] * padded[first : first + seq, :]
    mixed[...] = (post_ref[...].astype(f32) * convolved).astype(bf16)
    loads[0].wait()

    def rows_of(core):
        return jnp.concatenate(
            [mixed[pl.ds(pl.multiple_of(yy * half + core * rows, rows), rows), :] for yy in range(2)], 0
        )

    pair_send[...] = jnp.dot(rows_of(1 - c), out_w[...], preferred_element_type=f32).astype(bf16)
    pair_copy = remote(pair_send, pair_in, proj_sem.at[0], proj_sem.at[1], at(sp, sibling))
    pair_copy.start()
    own_sum[...] = jnp.dot(rows_of(c), out_w[...], preferred_element_type=f32)
    pair_copy.wait()
    far = pl.ds(pl.multiple_of((1 - y) * rows, rows), rows)
    near = pl.ds(pl.multiple_of(y * rows, rows), rows)
    y_send[...] = (own_sum[far, :] + pair_in[far, :].astype(f32)).astype(bf16)
    y_copy = remote(y_send, y_in, proj_sem.at[2], proj_sem.at[3], at(sp, opposite))
    y_copy.start()
    own_sum[near, :] = own_sum[near, :] + pair_in[near, :].astype(f32)
    y_copy.wait()
    residual = (stream_ref[...].astype(f32) + (own_sum[near, :] + y_in[...].astype(f32))).astype(bf16)
    resid[...] = residual
    tokens[sp, pl.ds(own_row, rows), :width] = scaled_norm(residual.astype(f32), gain_ref[...]).astype(bf16)

    own_block = tokens.at[sp, pl.ds(own_row, rows), :]
    block_copy = remote(own_block, own_block, y_sem.at[0], y_sem.at[1], at(sp, opposite))
    block_copy.start()

    def pair_of(group, core):
        return tokens.at[group, pl.ds(pl.multiple_of(core * half, half), half), :]

    def forward(way, group):
        device = (
            at(lax.rem(sp + 2, sp_count), tp),
            at(lax.rem(sp + sp_count - 2, sp_count), tp),
            at(across, tp),
            at(sp, sibling),
        )[way]
        pair = pair_of(group, c)
        return remote(pair, pair, tok_send.at[way, group], tok_recv.at[group, c], device)

    def arrival(group, core):
        pair = pair_of(group, core)
        return remote(pair, pair, tok_send.at[0, group], tok_recv.at[group, core], at(sp, sibling))

    def share(way, group):
        whose = tp if way < 2 else opposite
        block = hidden.at[group, whose]
        return remote(
            block, block, hid_send.at[way, group], hid_recv.at[group, whose], at(sp, sibling if way else opposite)
        )

    def shared(group, whose):
        block = hidden.at[group, whose]
        return remote(block, block, hid_send.at[0, group], hid_recv.at[group, whose], at(sp, sibling))

    near_first = [sorted(range(heights), key=lambda other: abs(other - i)) for i in range(heights)]
    far_first = [sorted(range(heights), key=lambda other: -abs(other - i)) for i in range(heights)]

    def group_at(tick):
        height = table_pick(near_first, z, lax.div(tick, 2))
        own_x = lax.rem(tick, 2) == 0
        return height, own_x, 2 * height + jnp.where(own_x, x, 1 - x)

    def homeward(group, down_side):
        device = at(lax.rem(sp + (sp_count - 2, 2)[down_side], sp_count), tp)
        return remote(
            part.at[group],
            chain_in.at[down_side, group],
            chain_send.at[group],
            chain_recv.at[down_side, group],
            device,
        )

    def send_home(group, height):
        @pl.when(height < z)
        def _():
            homeward(group, 0).start()

        @pl.when(height > z)
        def _():
            homeward(group, 1).start()

    last = heights - 1

    def incoming(height):
        return ((height < z) & (z < last)) | ((height > z) & (z > 0))

    def take_tokens(tick):
        height, own_x, group = group_at(tick)

        @pl.when(tick == 0)
        def _():
            block_copy.wait_recv()

        @pl.when(tick > 0)
        def _():
            arrival(group, c).wait_recv()

        @pl.when(own_x)
        def _():
            @pl.when((height <= z) & (z < last))
            def _():
                forward(0, group).start()

            @pl.when((height >= z) & (z > 0))
            def _():
                forward(1, group).start()

            forward(2, group).start()

        forward(3, group).start()
        arrival(group, 1 - c).wait_recv()

    def gated_units(tick):
        _, _, group = group_at(tick)
        inputs = tokens[group, :, :width]
        tile = min(256, units)
        for start in range(0, units, tile):
            gate_pre = jnp.dot(inputs, gate_w[:, start : start + tile], preferred_element_type=f32)
            up_pre = jnp.dot(inputs, up_w[:, start : start + tile], preferred_element_type=f32)
            hidden[group, tp, :, start : start + tile] = clamped_units(gate_pre, up_pre).astype(bf16)
        share(0, group).start()
        share(1, group).start()

    def relay_units(tick):
        _, _, group = group_at(tick)
        shared(group, opposite).wait_recv()
        share(2, group).start()

    def project_down(tick):
        height, _, group = group_at(tick)
        shared(group, sibling).wait_recv()
        shared(group, 3 - tp).wait_recv()
        total = jnp.dot(hidden[group, 0], down_w[:units, :], preferred_element_type=f32)
        for k in range(1, 4):
            total = total + jnp.dot(
                hidden[group, k], down_w[k * units : (k + 1) * units, :], preferred_element_type=f32
            )
        lanes = lax.broadcasted_iota(jnp.int32, (seq, LANES), 1)
        mine = (lanes == sp) | (lanes == sp + sp_count)
        scale = jnp.sum(jnp.where(mine, tokens[group, :, width:].astype(f32), 0.0), axis=1, keepdims=True)
        part[group] = (total.astype(bf16).astype(f32) * scale).astype(bf16)

        @pl.when(jnp.logical_not(incoming(height)))
        def _():
            send_home(group, height)

    for load in loads[1:]:
        load.wait()

    def tick_body(tick, carry):
        @pl.when(tick < sp_count)
        def _():
            take_tokens(tick)
            gated_units(tick)

        @pl.when((tick >= 1) & (tick < sp_count + 1))
        def _():
            relay_units(tick - 1)

        @pl.when(tick >= 2)
        def _():
            project_down(tick - 2)

        return carry

    lax.fori_loop(0, sp_count + 2, tick_body, 0)

    def came(down_side, group):
        return remote(
            part.at[group],
            chain_in.at[down_side, group],
            chain_send.at[group],
            chain_recv.at[down_side, group],
            at(sp, sibling),
        )

    def add_in(down_side, group):
        came(down_side, group).wait_recv()
        part[group] = (part[group].astype(f32) + chain_in[down_side, group].astype(f32)).astype(bf16)

    def chain_body(item, carry):
        height = table_pick(far_first, z, lax.div(item, 2))
        group = 2 * height + lax.rem(item, 2)

        @pl.when(incoming(height))
        def _():
            @pl.when(height < z)
            def _():
                add_in(0, group)

            @pl.when(height > z)
            def _():
                add_in(1, group)

            send_home(group, height)

        return carry

    lax.fori_loop(0, sp_count - 2, chain_body, 0)
    other = 2 * z + 1 - x
    x_copy = remote(part.at[other], x_in, x_sem.at[0], x_sem.at[1], at(across, tp))
    for group in (other, sp):
        @pl.when(z < last)
        def _():
            add_in(0, group)

        @pl.when(z > 0)
        def _():
            add_in(1, group)

        if group is other:
            x_copy.start()
    x_copy.wait_recv()
    final[...] = (part[sp].astype(f32) + x_in[...].astype(f32)).astype(bf16)

    def hand_over(step):
        to = lax.rem(tp + step, 4)
        begin = pl.multiple_of(lax.rem(to, 2) * half + lax.div(to, 2) * rows, rows)
        return remote(
            final.at[pl.ds(begin, rows), :], columns.at[tp], fin_send.at[step - 1], fin_recv.at[tp], at(sp, to)
        )

    for step in (1, 2, 3):
        hand_over(step).start()
    columns[tp] = final[pl.ds(own_row, rows), :]
    for step in (1, 2, 3):
        whose = lax.rem(tp + step, 4)
        remote(
            final.at[pl.ds(0, rows), :], columns.at[whose], fin_send.at[step - 1], fin_recv.at[whose], at(sp, sibling)
        ).wait_recv()
    combined = jnp.concatenate([columns[k] for k in range(4)], 1).astype(f32)
    result_ref[...] = (resid[...].astype(f32) + scaled_norm(combined, post_gain_ref[...])).astype(bf16)

    block_copy.wait_send()
    for step in (1, 2, 3):
        hand_over(step).wait_send()
    x_copy.wait_send()

    def drain(group, carry):
        height = lax.div(group, 2)

        @pl.when(lax.rem(group, 2) == x)
        def _():
            @pl.when((height <= z) & (z < last))
            def _():
                forward(0, group).wait_send()

            @pl.when((height >= z) & (z > 0))
            def _():
                forward(1, group).wait_send()

            forward(2, group).wait_send()

        forward(3, group).wait_send()
        for way in range(3):
            share(way, group).wait_send()

        @pl.when(height != z)
        def _():
            homeward(group, 0).wait_send()

        return carry

    lax.fori_loop(0, sp_count, drain, 0)


def dense_layer(
    stream_in,
    pre_gate,
    value_in,
    post_gate,
    conv_taps,
    out_weight,
    route_ids,
    route_weight,
    ffn_gain,
    post_gain,
    gate_proj,
    up_proj,
    down_proj,
):
    sp_count = lax.axis_size("sp")
    rows, width = stream_in.shape
    seq, channels = pre_gate.shape
    units = gate_proj.shape[2]
    cols = down_proj.shape[2]
    bf16, f32 = jnp.bfloat16, jnp.float32
    dma = pltpu.SemaphoreType.DMA
    scratch = [
        pltpu.VMEM(out_weight.shape, bf16),
        pltpu.VMEM(gate_proj.shape[1:], bf16),
        pltpu.VMEM(up_proj.shape[1:], bf16),
        pltpu.VMEM(down_proj.shape[1:], bf16),
        pltpu.VMEM((16, channels), bf16),
        pltpu.VMEM((16, channels), bf16),
        pltpu.VMEM((seq + 8, channels), f32),
        pltpu.VMEM((seq, channels), bf16),
        pltpu.VMEM((2 * rows, width), bf16),
        pltpu.VMEM((2 * rows, width), bf16),
        pltpu.VMEM((2 * rows, width), f32),
        pltpu.VMEM((rows, width), bf16),
        pltpu.VMEM((rows, width), bf16),
        pltpu.VMEM((rows, width), bf16),
        pltpu.VMEM((sp_count, seq, width + LANES), bf16),
        pltpu.VMEM((sp_count, 4, seq, units), bf16),
        pltpu.VMEM((sp_count, seq, cols), bf16),
        pltpu.VMEM((2, sp_count, seq, cols), bf16),
        pltpu.VMEM((seq, cols), bf16),
        pltpu.VMEM((seq, cols), bf16),
        pltpu.VMEM((4, rows, cols), bf16),
        dma((4,)),
        dma((2,)),
        dma((4,)),
        dma((2,)),
        dma((4, sp_count)),
        dma((sp_count, 2)),
        dma((3, sp_count)),
        dma((sp_count, 4)),
        dma((sp_count,)),
        dma((2, sp_count)),
        dma((2,)),
        dma((3,)),
        dma((4,)),
    ]
    vmem = pl.BlockSpec(memory_space=pltpu.VMEM)
    anywhere = pl.BlockSpec(memory_space=pl.ANY)
    return pl.pallas_call(
        functools.partial(layer_kernel, sp_count),
        out_shape=jax.ShapeDtypeStruct((rows, width), bf16),
        in_specs=[vmem] * 9 + [anywhere] * 4,
        out_specs=vmem,
        scratch_shapes=scratch,
        compiler_params=pltpu.CompilerParams(
            collective_id=0, has_side_effects=True, vmem_limit_bytes=58 * 1024 * 1024
        ),
    )(
        stream_in,
        pre_gate,
        value_in,
        post_gate,
        conv_taps,
        route_ids,
        route_weight,
        ffn_gain.reshape(1, -1),
        post_gain.reshape(1, -1),
        out_weight,
        gate_proj,
        up_proj,
        down_proj,
    )


def local(
    stream_in,
    pre_gate,
    value_in,
    post_gate,
    conv_taps,
    out_weight,
    route_ids,
    route_weight,
    ffn_gain,
    post_gain,
    gate_proj,
    up_proj,
    down_proj,
):
    sp_count = lax.axis_size("sp")
    tp_count = lax.axis_size("tp")
    seq_rows = pre_gate.shape[0]
    own_rows = seq_rows // tp_count
    top_count = route_ids.shape[1]
    slots_each = 2 * own_rows * top_count // sp_count
    if tp_count == 4 and sp_count % 2 == 0 and slots_each >= own_rows:
        return dense_layer(
            stream_in, pre_gate, value_in, post_gate, conv_taps, out_weight, route_ids, route_weight,
            ffn_gain, post_gain, gate_proj, up_proj, down_proj,
        )
    tap_count = conv_taps.shape[0]
    gated_input = (pre_gate.astype(jnp.float32) * value_in.astype(jnp.float32)).astype(jnp.bfloat16)
    rim_rows = passed_along(gated_input[seq_rows - tap_count + 1 :], "sp", 1)
    padded = jnp.concatenate([rim_rows, gated_input], 0).astype(jnp.float32)
    convolved = jnp.zeros(gated_input.shape, jnp.float32)
    for tap_index in range(tap_count):
        convolved = (
            convolved
            + conv_taps[tap_index].astype(jnp.float32)[None, :]
            * padded[tap_index : tap_index + seq_rows]
        )
    mixer_out = (post_gate.astype(jnp.float32) * convolved).astype(jnp.bfloat16)
    weight_rows = mixer_out
    projected = lax.psum_scatter(
        jnp.dot(weight_rows, out_weight, preferred_element_type=jnp.float32),
        "tp",
        scatter_dimension=0,
        tiled=True,
    )
    residual = (stream_in.astype(jnp.float32) + projected).astype(jnp.bfloat16)
    normed = scaled_norm(residual.astype(jnp.float32), ffn_gain).astype(jnp.bfloat16)
    slot_rank = block_ranks(route_ids, sp_count, own_rows)
    block_of = (jnp.arange(seq_rows, dtype=jnp.int32) // own_rows)[:, None]
    tp_index = lax.axis_index("tp")
    own_ids = lax.dynamic_slice_in_dim(route_ids, tp_index * own_rows, own_rows, 0)
    own_rank = lax.dynamic_slice_in_dim(slot_rank, tp_index * own_rows, own_rows, 0)
    own_slot = own_ids * slots_each + own_rank
    picker = slot_picker(own_slot, sp_count * slots_each)
    outgoing = jnp.dot(picker, normed, preferred_element_type=jnp.float32).astype(jnp.bfloat16)
    arrived = lax.all_to_all(outgoing, "sp", split_axis=0, concat_axis=0, tiled=True)
    portion = lax.all_gather(arrived, "tp", axis=0, tiled=True)
    gate_pre = jnp.dot(portion, gate_proj[0], preferred_element_type=jnp.float32)
    up_pre = jnp.dot(portion, up_proj[0], preferred_element_type=jnp.float32)
    hidden = clamped_units(gate_pre, up_pre).astype(jnp.bfloat16)
    weight_rows = down_proj[0]
    column_out = jnp.dot(
        lax.all_gather(hidden, "tp", axis=1, tiled=True),
        weight_rows,
        preferred_element_type=jnp.float32,
    ).astype(jnp.bfloat16)
    column_width = column_out.shape[1]
    returned = lax.all_to_all(
        column_out.reshape(tp_count, sp_count, slots_each, column_width),
        "sp",
        split_axis=1,
        concat_axis=1,
        tiled=True,
    )
    home_index = (block_of * sp_count + route_ids) * slots_each + slot_rank
    gathered_out = jnp.take(returned.reshape(-1, column_width), home_index.reshape(-1), axis=0)
    gathered_out = gathered_out.astype(jnp.float32).reshape(seq_rows, top_count, column_width)
    combined_cols = jnp.sum(gathered_out * route_weight[:, :, None], axis=1).astype(jnp.bfloat16)
    combined = lax.all_to_all(combined_cols, "tp", split_axis=0, concat_axis=1, tiled=True)
    layer_out = residual.astype(jnp.float32) + scaled_norm(combined.astype(jnp.float32), post_gain)
    return layer_out.astype(jnp.bfloat16)


def solution(mesh):
    placed = (
        P(("sp", "tp"), None),
        P("sp", "tp"),
        P("sp", "tp"),
        P("sp", "tp"),
        P(None, "tp"),
        P("tp", None),
        P("sp", None),
        P("sp", None),
        P(),
        P(),
        P("sp", None, "tp"),
        P("sp", None, "tp"),
        P("sp", None, "tp"),
    )
    return jax.shard_map(
        local, mesh=mesh, in_specs=placed, out_specs=P(("sp", "tp"), None), check_vma=False
    )
```

```python
import functools

import jax
import jax.numpy as jnp
from jax import lax
from jax.experimental import pallas as pl
from jax.experimental.pallas import tpu as pltpu
from jax.sharding import PartitionSpec as P

clamp_limit = 7.0
sigmoid_scale = 1.702
epsilon = 1e-06


def passed_along(array, axis, by):
    count = lax.axis_size(axis)
    pairs = [(i, i + by) for i in range(count) if 0 <= i + by < count]
    return lax.ppermute(array, axis, pairs)


def clamped_units(gate_pre, up_pre):
    gate_cut = jnp.minimum(gate_pre, clamp_limit)
    up_cut = jnp.clip(up_pre, -clamp_limit, clamp_limit)
    return (up_cut + 1.0) * (gate_cut * jax.nn.sigmoid(sigmoid_scale * gate_cut))


def scaled_norm(values, gain):
    return (
        values
        * lax.rsqrt(jnp.mean(values * values, axis=-1, keepdims=True) + epsilon)
        * gain.astype(jnp.float32)
    )


def block_ranks(route_rows, experts, block_rows):
    flattened = route_rows.reshape(-1)
    entries = flattened.shape[0]
    span_width = block_rows * route_rows.shape[1]
    onehot = (flattened[:, None] == jnp.arange(experts, dtype=jnp.int32)[None, :]).astype(jnp.int32)
    blocked = onehot.reshape(entries // span_width, span_width, experts)
    before = jnp.cumsum(blocked, axis=1) - blocked
    return jnp.sum(before * blocked, axis=2).reshape(route_rows.shape)


def slot_picker(slot_index, table_size):
    matches = slot_index[None, :, :] == jnp.arange(table_size, dtype=jnp.int32)[:, None, None]
    return jnp.any(matches, axis=2).astype(jnp.bfloat16)


LANES = 128


def table_pick(table, first, second):
    value = jnp.int32(0)
    for i, row in enumerate(table):
        for j, entry in enumerate(row):
            if entry:
                value = value + jnp.where((first == i) & (second == j), entry, 0)
    return value


def layer_kernel(
    sp_count,
    stream_ref,
    pre_ref,
    value_ref,
    post_ref,
    taps_ref,
    ids_ref,
    weight_ref,
    gain_ref,
    post_gain_ref,
    out_hbm,
    gate_hbm,
    up_hbm,
    down_hbm,
    result_ref,
    out_w,
    gate_w,
    up_w,
    down_w,
    tail,
    rim,
    padded,
    mixed,
    pair_send,
    pair_in,
    own_sum,
    y_send,
    y_in,
    resid,
    tokens,
    hidden,
    part,
    chain_in,
    x_in,
    final,
    columns,
    load_sem,
    rim_sem,
    proj_sem,
    y_sem,
    tok_send,
    tok_recv,
    hid_send,
    hid_recv,
    chain_send,
    chain_recv,
    x_sem,
    fin_send,
    fin_recv,
):
    f32, bf16 = jnp.float32, jnp.bfloat16
    heights = sp_count // 2
    sp = lax.axis_index("sp")
    tp = lax.axis_index("tp")
    z, x = lax.div(sp, 2), lax.rem(sp, 2)
    y, c = lax.div(tp, 2), lax.rem(tp, 2)
    across, sibling = sp + 1 - 2 * x, tp + 1 - 2 * c
    opposite = lax.rem(tp + 2, 4)
    rows, width = stream_ref.shape
    seq = 4 * rows
    half = 2 * rows
    units = gate_w.shape[1]

    def at(sp_to, tp_to):
        return {"sp": sp_to, "tp": tp_to}

    def remote(source, target, send, receive, device):
        return pltpu.make_async_remote_copy(
            src_ref=source,
            dst_ref=target,
            send_sem=send,
            recv_sem=receive,
            device_id=device,
            device_id_type=pl.DeviceIdType.MESH,
        )

    loads = [
        pltpu.make_async_copy(source, target, load_sem.at[i])
        for i, (source, target) in enumerate(
            ((out_hbm, out_w), (gate_hbm.at[0], gate_w), (up_hbm.at[0], up_w), (down_hbm.at[0], down_w))
        )
    ]
    for load in loads:
        load.start()

    barrier = pltpu.get_barrier_semaphore()
    partners = [at(lax.rem(sp + by, sp_count), tp) for by in (1, 2, sp_count - 1, sp_count - 2)]
    partners += [at(across, tp), at(sp, sibling), at(sp, opposite), at(sp, 3 - tp)]
    for partner in partners:
        pl.semaphore_signal(barrier, inc=1, device_id=partner, device_id_type=pl.DeviceIdType.MESH)
    pl.semaphore_wait(barrier, len(partners))

    gated = (pre_ref[...].astype(f32) * value_ref[...].astype(f32)).astype(bf16)
    tail[...] = gated[seq - 16 :]
    rim_copy = remote(tail, rim, rim_sem.at[0], rim_sem.at[1], at(lax.rem(sp + 1, sp_count), tp))
    rim_copy.start()
    padded[8:, :] = gated.astype(f32)
    lane = lax.broadcasted_iota(jnp.int32, (rows, LANES), 1)
    row = lax.broadcasted_iota(jnp.int32, (rows, seq), 0)
    picked = (lax.broadcasted_iota(jnp.int32, (rows, seq), 1) == row + tp * rows).astype(bf16)

    def own_columns(values):
        return lax.dot_general(picked, values, (((1,), (1,)), ((), ())), preferred_element_type=f32)

    top_count = ids_ref.shape[0]
    weights = weight_ref[...]
    high = weights.astype(bf16)
    low = own_columns((weights - high.astype(f32)).astype(bf16))
    high = own_columns(high)
    ids = own_columns(ids_ref[...].astype(f32).astype(bf16)).astype(jnp.int32)
    spread = jnp.zeros((rows, LANES), f32)
    for k in range(top_count):
        spread = spread + jnp.where(lane == ids[:, k : k + 1], high[:, k : k + 1], 0.0)
        spread = spread + jnp.where(lane == ids[:, k : k + 1] + sp_count, low[:, k : k + 1], 0.0)
    own_row = pl.multiple_of(c * half + y * rows, rows)
    tokens[sp, pl.ds(own_row, rows), width:] = spread.astype(bf16)
    rim_copy.wait()
    padded[:8, :] = jnp.where(sp == 0, 0.0, rim[...].astype(f32)[8:])
    tap_count = taps_ref.shape[0]
    taps = taps_ref[...].astype(f32)
    convolved = jnp.zeros((seq, padded.shape[1]), f32)
    for k in range(tap_count):
        first = 8 - tap_count + 1 + k
        convolved = convolved + taps[k : k + 1, :] * padded[first : first + seq, :]
    mixed[...] = (post_ref[...].astype(f32) * convolved).astype(bf16)
    loads[0].wait()

    def rows_of(core):
        return jnp.concatenate(
            [mixed[pl.ds(pl.multiple_of(yy * half + core * rows, rows), rows), :] for yy in range(2)], 0
        )

    pair_send[...] = jnp.dot(rows_of(1 - c), out_w[...], preferred_element_type=f32).astype(bf16)
    pair_copy = remote(pair_send, pair_in, proj_sem.at[0], proj_sem.at[1], at(sp, sibling))
    pair_copy.start()
    own_sum[...] = jnp.dot(rows_of(c), out_w[...], preferred_element_type=f32)
    pair_copy.wait()
    far = pl.ds(pl.multiple_of((1 - y) * rows, rows), rows)
    near = pl.ds(pl.multiple_of(y * rows, rows), rows)
    y_send[...] = (own_sum[far, :] + pair_in[far, :].astype(f32)).astype(bf16)
    y_copy = remote(y_send, y_in, proj_sem.at[2], proj_sem.at[3], at(sp, opposite))
    y_copy.start()
    own_sum[near, :] = own_sum[near, :] + pair_in[near, :].astype(f32)
    y_copy.wait()
    residual = (stream_ref[...].astype(f32) + (own_sum[near, :] + y_in[...].astype(f32))).astype(bf16)
    resid[...] = residual
    tokens[sp, pl.ds(own_row, rows), :width] = scaled_norm(residual.astype(f32), gain_ref[...].reshape(1, width)).astype(bf16)

    def block_of(group, slot):
        return tokens.at[group, pl.ds(pl.multiple_of(slot * rows, rows), rows), :]

    own_block = block_of(sp, 2 * c + y)
    block_copy = remote(own_block, own_block, y_sem.at[0], tok_recv.at[sp, 2 * c + y], at(sp, opposite))

    def forward(way, group, yy):
        device = (
            at(lax.rem(sp + 2, sp_count), tp),
            at(lax.rem(sp + sp_count - 2, sp_count), tp),
            at(across, tp),
            at(sp, sibling),
        )[way]
        block = block_of(group, 2 * c + yy)
        return remote(block, block, tok_send.at[way, group, yy], tok_recv.at[group, 2 * c + yy], device)

    def arrival(group, slot):
        block = block_of(group, slot)
        return remote(block, block, y_sem.at[0], tok_recv.at[group, slot], at(sp, sibling))

    def share(way, group):
        whose = tp if way < 2 else opposite
        block = hidden.at[group, whose]
        return remote(
            block, block, hid_send.at[way, group], hid_recv.at[group, whose], at(sp, sibling if way else opposite)
        )

    def shared(group, whose):
        block = hidden.at[group, whose]
        return remote(block, block, hid_send.at[0, group], hid_recv.at[group, whose], at(sp, sibling))

    near_first = [sorted(range(heights), key=lambda other: abs(other - i)) for i in range(heights)]
    home_order = [
        sorted(
            range(heights),
            key=lambda other: (other == i, heights - 1 - i if other < i else i, abs(other - i)),
        )
        for i in range(heights)
    ]

    def group_at(tick):
        height = table_pick(near_first, z, lax.div(tick, 2))
        own_x = lax.rem(tick, 2) == 0
        return height, 2 * height + jnp.where(own_x, x, 1 - x)

    def half_of(part_number):
        return pl.ds(part_number * half, half)

    def homeward(group, down_side, h):
        device = at(lax.rem(sp + (sp_count - 2, 2)[down_side], sp_count), tp)
        return remote(
            part.at[group, half_of(h), :],
            chain_in.at[down_side, group, half_of(h), :],
            chain_send.at[group, h],
            chain_recv.at[down_side, group, h],
            device,
        )

    def send_home(group, height, h):
        @pl.when(height < z)
        def _():
            homeward(group, 0, h).start()

        @pl.when(height > z)
        def _():
            homeward(group, 1, h).start()

    last = heights - 1

    def incoming(height):
        return ((height < z) & (z < last)) | ((height > z) & (z > 0))

    def own_side(step):
        height = table_pick(near_first, z, lax.div(step, 2))
        return height, jnp.where(lax.rem(step, 2) == 0, y, 1 - y)

    def take_own(height, yy):
        group = 2 * height + x
        arrival(group, 2 * c + yy).wait_recv()

        @pl.when((height <= z) & (z < last))
        def _():
            forward(0, group, yy).start()

        @pl.when((height >= z) & (z > 0))
        def _():
            forward(1, group, yy).start()

        forward(3, group, yy).start()

    def send_across(step):
        height, yy = own_side(step)
        forward(2, 2 * height + x, yy).start()

    def take_across(step):
        height, yy = own_side(step)
        group = 2 * height + 1 - x
        arrival(group, 2 * c + yy).wait_recv()
        forward(3, group, yy).start()

    def gated_units(tick):
        _, group = group_at(tick)
        for yy in range(2):
            arrival(group, 2 * (1 - c) + yy).wait_recv()
        inputs = tokens[group, :, :width]
        tile = min(256, units)
        for start in range(0, units, tile):
            gate_pre = jnp.dot(inputs, gate_w[:, start : start + tile], preferred_element_type=f32)
            up_pre = jnp.dot(inputs, up_w[:, start : start + tile], preferred_element_type=f32)
            hidden[group, tp, :, start : start + tile] = clamped_units(gate_pre, up_pre).astype(bf16)
        share(0, group).start()
        share(1, group).start()

    def relay_units(tick):
        _, group = group_at(tick)
        shared(group, opposite).wait_recv()
        share(2, group).start()

    def project_down(tick):
        height, group = group_at(tick)
        shared(group, sibling).wait_recv()
        shared(group, 3 - tp).wait_recv()
        total = jnp.dot(hidden[group, 0], down_w[:units, :], preferred_element_type=f32)
        for k in range(1, 4):
            total = total + jnp.dot(
                hidden[group, k], down_w[k * units : (k + 1) * units, :], preferred_element_type=f32
            )
        lanes = lax.broadcasted_iota(jnp.int32, (seq, LANES), 1)
        mine = (lanes == sp) | (lanes == sp + sp_count)
        scale = jnp.sum(jnp.where(mine, tokens[group, :, width:].astype(f32), 0.0), axis=1, keepdims=True)
        part[group] = (total.astype(bf16).astype(f32) * scale).astype(bf16)

        @pl.when(jnp.logical_not(incoming(height)))
        def _():
            for h in range(2):
                send_home(group, height, h)

    block_copy.start()
    for way, there in ((0, z < last), (1, z > 0)):

        @pl.when(there)
        def _():
            forward(way, sp, y).start()

    forward(2, sp, y).start()
    forward(3, sp, y).start()
    take_own(z, 1 - y)
    send_across(jnp.int32(1))
    for load in loads[1:]:
        load.wait()

    def take_step(step, yy):
        distance = lax.div(step, 2) + 1

        @pl.when(z >= distance)
        def _():
            take_own(z - distance, yy)

        @pl.when(z + distance <= last)
        def _():
            take_own(z + distance, yy)

        send_across(step + 2)

    gated_units(jnp.int32(0))

    def round_body(j, carry):
        early, late = 2 * j, 2 * j + 1

        @pl.when(j < last)
        def _():
            take_step(early, y)

        take_across(early)

        @pl.when(j >= 1)
        def _():
            relay_units(early - 1)
            project_down(early - 2)

        @pl.when(j < last)
        def _():
            take_step(late, 1 - y)

        take_across(late)
        gated_units(late)

        @pl.when(j < last)
        def _():
            gated_units(late + 1)

        relay_units(early)

        @pl.when(j >= 1)
        def _():
            project_down(early - 1)

        return carry

    lax.fori_loop(0, heights, round_body, 0)
    relay_units(sp_count - 1)
    project_down(sp_count - 2)
    project_down(sp_count - 1)

    def add_in(down_side, group, h):
        remote(
            part.at[group, half_of(h), :],
            chain_in.at[down_side, group, half_of(h), :],
            chain_send.at[group, h],
            chain_recv.at[down_side, group, h],
            at(sp, sibling),
        ).wait_recv()
        part[group, half_of(h), :] = (
            part[group, half_of(h), :].astype(f32) + chain_in[down_side, group, half_of(h), :].astype(f32)
        ).astype(bf16)

    def chain_body(item, carry):
        height = table_pick(home_order, z, lax.div(item, 2))
        group = 2 * height + jnp.where(lax.rem(item, 2) == 0, x, 1 - x)

        @pl.when(incoming(height))
        def _():
            for h in range(2):

                @pl.when(height < z)
                def _():
                    add_in(0, group, h)

                @pl.when(height > z)
                def _():
                    add_in(1, group, h)

                send_home(group, height, h)

        return carry

    lax.fori_loop(0, sp_count - 2, chain_body, 0)
    other = 2 * z + 1 - x

    def both_sides(group, h):
        @pl.when(z < last)
        def _():
            add_in(0, group, h)

        @pl.when(z > 0)
        def _():
            add_in(1, group, h)

    def over_x(h):
        return remote(
            part.at[other, half_of(h), :], x_in.at[half_of(h), :], x_sem.at[0, h], x_sem.at[1, h], at(across, tp)
        )

    def hand_over(h, yy):
        return remote(
            final.at[pl.ds(h * half + yy * rows, rows), :],
            columns.at[tp],
            fin_send.at[2 * h + yy],
            fin_recv.at[tp],
            at(sp, 2 * yy + h),
        )

    for h in range(2):
        both_sides(other, h)
        over_x(h).start()
    for h in range(2):
        both_sides(sp, h)
        over_x(h).wait_recv()
        final[half_of(h), :] = (part[sp, half_of(h), :].astype(f32) + x_in[half_of(h), :].astype(f32)).astype(bf16)
        for yy in range(2):

            @pl.when(tp != 2 * yy + h)
            def _():
                hand_over(h, yy).start()

    columns[tp] = final[pl.ds(own_row, rows), :]
    for step in (1, 2, 3):
        whose = lax.rem(tp + step, 4)
        remote(
            final.at[pl.ds(0, rows), :], columns.at[whose], fin_send.at[0], fin_recv.at[whose], at(sp, sibling)
        ).wait_recv()
    combined = jnp.concatenate([columns[k] for k in range(4)], 1).astype(f32)
    result_ref[...] = (
        resid[...].astype(f32) + scaled_norm(combined, post_gain_ref[...].reshape(1, width))
    ).astype(bf16)

    block_copy.wait_send()
    for h in range(2):
        over_x(h).wait_send()
        for yy in range(2):

            @pl.when(tp != 2 * yy + h)
            def _():
                hand_over(h, yy).wait_send()

    def drain(group, carry):
        height = lax.div(group, 2)

        for yy in range(2):

            @pl.when(lax.rem(group, 2) == x)
            def _():
                @pl.when((height <= z) & (z < last))
                def _():
                    forward(0, group, yy).wait_send()

                @pl.when((height >= z) & (z > 0))
                def _():
                    forward(1, group, yy).wait_send()

                forward(2, group, yy).wait_send()

            forward(3, group, yy).wait_send()
        for way in range(3):
            share(way, group).wait_send()

        @pl.when(height != z)
        def _():
            for h in range(2):
                homeward(group, 0, h).wait_send()

        return carry

    lax.fori_loop(0, sp_count, drain, 0)


def dense_layer(
    stream_in,
    pre_gate,
    value_in,
    post_gate,
    conv_taps,
    out_weight,
    route_ids,
    route_weight,
    ffn_gain,
    post_gain,
    gate_proj,
    up_proj,
    down_proj,
):
    sp_count = lax.axis_size("sp")
    rows, width = stream_in.shape
    seq, channels = pre_gate.shape
    units = gate_proj.shape[2]
    cols = down_proj.shape[2]
    bf16, f32 = jnp.bfloat16, jnp.float32
    dma = pltpu.SemaphoreType.DMA
    scratch = [
        pltpu.VMEM(out_weight.shape, bf16),
        pltpu.VMEM(gate_proj.shape[1:], bf16),
        pltpu.VMEM(up_proj.shape[1:], bf16),
        pltpu.VMEM(down_proj.shape[1:], bf16),
        pltpu.VMEM((16, channels), bf16),
        pltpu.VMEM((16, channels), bf16),
        pltpu.VMEM((seq + 8, channels), f32),
        pltpu.VMEM((seq, channels), bf16),
        pltpu.VMEM((2 * rows, width), bf16),
        pltpu.VMEM((2 * rows, width), bf16),
        pltpu.VMEM((2 * rows, width), f32),
        pltpu.VMEM((rows, width), bf16),
        pltpu.VMEM((rows, width), bf16),
        pltpu.VMEM((rows, width), bf16),
        pltpu.VMEM((sp_count, seq, width + LANES), bf16),
        pltpu.VMEM((sp_count, 4, seq, units), bf16),
        pltpu.VMEM((sp_count, seq, cols), bf16),
        pltpu.VMEM((2, sp_count, seq, cols), bf16),
        pltpu.VMEM((seq, cols), bf16),
        pltpu.VMEM((seq, cols), bf16),
        pltpu.VMEM((4, rows, cols), bf16),
        dma((4,)),
        dma((2,)),
        dma((4,)),
        dma((1,)),
        dma((4, sp_count, 2)),
        dma((sp_count, 4)),
        dma((3, sp_count)),
        dma((sp_count, 4)),
        dma((sp_count, 2)),
        dma((2, sp_count, 2)),
        dma((2, 2)),
        dma((4,)),
        dma((4,)),
    ]
    vmem = pl.BlockSpec(memory_space=pltpu.VMEM)
    anywhere = pl.BlockSpec(memory_space=pl.ANY)
    return pl.pallas_call(
        functools.partial(layer_kernel, sp_count),
        out_shape=jax.ShapeDtypeStruct((rows, width), bf16),
        in_specs=[vmem] * 9 + [anywhere] * 4,
        out_specs=vmem,
        scratch_shapes=scratch,
        compiler_params=pltpu.CompilerParams(
            collective_id=0, has_side_effects=True, vmem_limit_bytes=58 * 1024 * 1024
        ),
    )(
        stream_in,
        pre_gate,
        value_in,
        post_gate,
        conv_taps,
        route_ids.T,
        route_weight.T,
        ffn_gain,
        post_gain,
        out_weight,
        gate_proj,
        up_proj,
        down_proj,
    )


def local(
    stream_in,
    pre_gate,
    value_in,
    post_gate,
    conv_taps,
    out_weight,
    route_ids,
    route_weight,
    ffn_gain,
    post_gain,
    gate_proj,
    up_proj,
    down_proj,
):
    sp_count = lax.axis_size("sp")
    tp_count = lax.axis_size("tp")
    seq_rows = pre_gate.shape[0]
    own_rows = seq_rows // tp_count
    top_count = route_ids.shape[1]
    slots_each = 2 * own_rows * top_count // sp_count
    if tp_count == 4 and sp_count % 2 == 0 and slots_each >= own_rows:
        return dense_layer(
            stream_in, pre_gate, value_in, post_gate, conv_taps, out_weight, route_ids, route_weight,
            ffn_gain, post_gain, gate_proj, up_proj, down_proj,
        )
    tap_count = conv_taps.shape[0]
    gated_input = (pre_gate.astype(jnp.float32) * value_in.astype(jnp.float32)).astype(jnp.bfloat16)
    rim_rows = passed_along(gated_input[seq_rows - tap_count + 1 :], "sp", 1)
    padded = jnp.concatenate([rim_rows, gated_input], 0).astype(jnp.float32)
    convolved = jnp.zeros(gated_input.shape, jnp.float32)
    for tap_index in range(tap_count):
        convolved = (
            convolved
            + conv_taps[tap_index].astype(jnp.float32)[None, :]
            * padded[tap_index : tap_index + seq_rows]
        )
    mixer_out = (post_gate.astype(jnp.float32) * convolved).astype(jnp.bfloat16)
    weight_rows = mixer_out
    projected = lax.psum_scatter(
        jnp.dot(weight_rows, out_weight, preferred_element_type=jnp.float32),
        "tp",
        scatter_dimension=0,
        tiled=True,
    )
    residual = (stream_in.astype(jnp.float32) + projected).astype(jnp.bfloat16)
    normed = scaled_norm(residual.astype(jnp.float32), ffn_gain).astype(jnp.bfloat16)
    slot_rank = block_ranks(route_ids, sp_count, own_rows)
    block_of = (jnp.arange(seq_rows, dtype=jnp.int32) // own_rows)[:, None]
    tp_index = lax.axis_index("tp")
    own_ids = lax.dynamic_slice_in_dim(route_ids, tp_index * own_rows, own_rows, 0)
    own_rank = lax.dynamic_slice_in_dim(slot_rank, tp_index * own_rows, own_rows, 0)
    own_slot = own_ids * slots_each + own_rank
    picker = slot_picker(own_slot, sp_count * slots_each)
    outgoing = jnp.dot(picker, normed, preferred_element_type=jnp.float32).astype(jnp.bfloat16)
    arrived = lax.all_to_all(outgoing, "sp", split_axis=0, concat_axis=0, tiled=True)
    portion = lax.all_gather(arrived, "tp", axis=0, tiled=True)
    gate_pre = jnp.dot(portion, gate_proj[0], preferred_element_type=jnp.float32)
    up_pre = jnp.dot(portion, up_proj[0], preferred_element_type=jnp.float32)
    hidden = clamped_units(gate_pre, up_pre).astype(jnp.bfloat16)
    weight_rows = down_proj[0]
    column_out = jnp.dot(
        lax.all_gather(hidden, "tp", axis=1, tiled=True),
        weight_rows,
        preferred_element_type=jnp.float32,
    ).astype(jnp.bfloat16)
    column_width = column_out.shape[1]
    returned = lax.all_to_all(
        column_out.reshape(tp_count, sp_count, slots_each, column_width),
        "sp",
        split_axis=1,
        concat_axis=1,
        tiled=True,
    )
    home_index = (block_of * sp_count + route_ids) * slots_each + slot_rank
    gathered_out = jnp.take(returned.reshape(-1, column_width), home_index.reshape(-1), axis=0)
    gathered_out = gathered_out.astype(jnp.float32).reshape(seq_rows, top_count, column_width)
    combined_cols = jnp.sum(gathered_out * route_weight[:, :, None], axis=1).astype(jnp.bfloat16)
    combined = lax.all_to_all(combined_cols, "tp", split_axis=0, concat_axis=1, tiled=True)
    layer_out = residual.astype(jnp.float32) + scaled_norm(combined.astype(jnp.float32), post_gain)
    return layer_out.astype(jnp.bfloat16)


def solution(mesh):
    placed = (
        P(("sp", "tp"), None),
        P("sp", "tp"),
        P("sp", "tp"),
        P("sp", "tp"),
        P(None, "tp"),
        P("tp", None),
        P("sp", None),
        P("sp", None),
        P(),
        P(),
        P("sp", None, "tp"),
        P("sp", None, "tp"),
        P("sp", None, "tp"),
    )
    return jax.shard_map(
        local, mesh=mesh, in_specs=placed, out_specs=P(("sp", "tp"), None), check_vma=False
    )
```

```python
import functools

import jax
import jax.numpy as jnp
from jax import lax
from jax.experimental import pallas as pl
from jax.experimental.pallas import tpu as pltpu
from jax.sharding import PartitionSpec as P

clamp_limit = 7.0
sigmoid_scale = 1.702
epsilon = 1e-06


def passed_along(array, axis, by):
    count = lax.axis_size(axis)
    pairs = [(i, i + by) for i in range(count) if 0 <= i + by < count]
    return lax.ppermute(array, axis, pairs)


def clamped_units(gate_pre, up_pre):
    gate_cut = jnp.minimum(gate_pre, clamp_limit)
    up_cut = jnp.clip(up_pre, -clamp_limit, clamp_limit)
    return (up_cut + 1.0) * (gate_cut * jax.nn.sigmoid(sigmoid_scale * gate_cut))


def scaled_norm(values, gain):
    return (
        values
        * lax.rsqrt(jnp.mean(values * values, axis=-1, keepdims=True) + epsilon)
        * gain.astype(jnp.float32)
    )


def block_ranks(route_rows, experts, block_rows):
    flattened = route_rows.reshape(-1)
    entries = flattened.shape[0]
    span_width = block_rows * route_rows.shape[1]
    onehot = (flattened[:, None] == jnp.arange(experts, dtype=jnp.int32)[None, :]).astype(jnp.int32)
    blocked = onehot.reshape(entries // span_width, span_width, experts)
    before = jnp.cumsum(blocked, axis=1) - blocked
    return jnp.sum(before * blocked, axis=2).reshape(route_rows.shape)


def slot_picker(slot_index, table_size):
    matches = slot_index[None, :, :] == jnp.arange(table_size, dtype=jnp.int32)[:, None, None]
    return jnp.any(matches, axis=2).astype(jnp.bfloat16)


LANES = 128


def table_pick(table, first, second):
    value = jnp.int32(0)
    for i, row in enumerate(table):
        for j, entry in enumerate(row):
            if entry:
                value = value + jnp.where((first == i) & (second == j), entry, 0)
    return value


def layer_kernel(
    sp_count,
    stream_ref,
    pre_ref,
    value_ref,
    post_ref,
    taps_ref,
    ids_ref,
    weight_ref,
    gain_ref,
    post_gain_ref,
    out_hbm,
    gate_hbm,
    up_hbm,
    down_hbm,
    result_ref,
    out_w,
    gate_w,
    up_w,
    down_w,
    tail,
    rim,
    padded,
    mixed,
    pair_send,
    pair_in,
    own_sum,
    y_send,
    y_in,
    resid,
    tokens,
    hidden,
    part,
    chain_in,
    x_in,
    final,
    columns,
    load_sem,
    rim_sem,
    proj_sem,
    y_sem,
    tok_send,
    tok_recv,
    hid_send,
    hid_recv,
    chain_send,
    chain_recv,
    x_send,
    x_recv,
    fin_send,
    fin_recv,
):
    f32, bf16 = jnp.float32, jnp.bfloat16
    heights = sp_count // 2
    sp = lax.axis_index("sp")
    tp = lax.axis_index("tp")
    z, x = lax.div(sp, 2), lax.rem(sp, 2)
    y, c = lax.div(tp, 2), lax.rem(tp, 2)
    across, sibling = sp + 1 - 2 * x, tp + 1 - 2 * c
    opposite = lax.rem(tp + 2, 4)
    rows, width = stream_ref.shape
    seq = 4 * rows
    half = 2 * rows
    units = gate_w.shape[1]

    def at(sp_to, tp_to):
        return {"sp": sp_to, "tp": tp_to}

    def remote(source, target, send, receive, device):
        return pltpu.make_async_remote_copy(
            src_ref=source,
            dst_ref=target,
            send_sem=send,
            recv_sem=receive,
            device_id=device,
            device_id_type=pl.DeviceIdType.MESH,
        )

    loads = [
        pltpu.make_async_copy(source, target, load_sem.at[i])
        for i, (source, target) in enumerate(
            ((out_hbm, out_w), (gate_hbm.at[0], gate_w), (up_hbm.at[0], up_w), (down_hbm.at[0], down_w))
        )
    ]
    for load in loads:
        load.start()

    barrier = pltpu.get_barrier_semaphore()
    partners = [at(lax.rem(sp + by, sp_count), tp) for by in (1, 2, sp_count - 1, sp_count - 2)]
    partners += [at(across, tp), at(sp, sibling), at(sp, opposite), at(sp, 3 - tp)]
    for partner in partners:
        pl.semaphore_signal(barrier, inc=1, device_id=partner, device_id_type=pl.DeviceIdType.MESH)
    pl.semaphore_wait(barrier, len(partners))

    gated = (pre_ref[...].astype(f32) * value_ref[...].astype(f32)).astype(bf16)
    tail[...] = gated[seq - 16 :]
    rim_copy = remote(tail, rim, rim_sem.at[0], rim_sem.at[1], at(lax.rem(sp + 1, sp_count), tp))
    rim_copy.start()
    padded[8:, :] = gated.astype(f32)
    lane = lax.broadcasted_iota(jnp.int32, (rows, LANES), 1)
    row = lax.broadcasted_iota(jnp.int32, (rows, seq), 0)
    picked = (lax.broadcasted_iota(jnp.int32, (rows, seq), 1) == row + tp * rows).astype(bf16)

    def own_columns(values):
        return lax.dot_general(picked, values, (((1,), (1,)), ((), ())), preferred_element_type=f32)

    top_count = ids_ref.shape[0]
    weights = weight_ref[...]
    high = weights.astype(bf16)
    low = own_columns((weights - high.astype(f32)).astype(bf16))
    high = own_columns(high)
    ids = own_columns(ids_ref[...].astype(f32).astype(bf16)).astype(jnp.int32)
    spread = jnp.zeros((rows, LANES), f32)
    for k in range(top_count):
        spread = spread + jnp.where(lane == ids[:, k : k + 1], high[:, k : k + 1], 0.0)
        spread = spread + jnp.where(lane == ids[:, k : k + 1] + sp_count, low[:, k : k + 1], 0.0)
    own_row = pl.multiple_of(c * half + y * rows, rows)
    tokens[sp, pl.ds(own_row, rows), width:] = spread.astype(bf16)
    rim_copy.wait()
    padded[:8, :] = jnp.where(sp == 0, 0.0, rim[...].astype(f32)[8:])
    tap_count = taps_ref.shape[0]
    taps = taps_ref[...].astype(f32)
    convolved = jnp.zeros((seq, padded.shape[1]), f32)
    for k in range(tap_count):
        first = 8 - tap_count + 1 + k
        convolved = convolved + taps[k : k + 1, :] * padded[first : first + seq, :]
    mixed[...] = (post_ref[...].astype(f32) * convolved).astype(bf16)
    loads[0].wait()

    def rows_of(core):
        return jnp.concatenate(
            [mixed[pl.ds(pl.multiple_of(yy * half + core * rows, rows), rows), :] for yy in range(2)], 0
        )

    pair_send[...] = jnp.dot(rows_of(1 - c), out_w[...], preferred_element_type=f32).astype(bf16)
    pair_copy = remote(pair_send, pair_in, proj_sem.at[0], proj_sem.at[1], at(sp, sibling))
    pair_copy.start()
    own_sum[...] = jnp.dot(rows_of(c), out_w[...], preferred_element_type=f32)
    pair_copy.wait()
    far = pl.ds(pl.multiple_of((1 - y) * rows, rows), rows)
    near = pl.ds(pl.multiple_of(y * rows, rows), rows)
    y_send[...] = (own_sum[far, :] + pair_in[far, :].astype(f32)).astype(bf16)
    y_copy = remote(y_send, y_in, proj_sem.at[2], proj_sem.at[3], at(sp, opposite))
    y_copy.start()
    own_sum[near, :] = own_sum[near, :] + pair_in[near, :].astype(f32)
    y_copy.wait()
    residual = (stream_ref[...].astype(f32) + (own_sum[near, :] + y_in[...].astype(f32))).astype(bf16)
    resid[...] = residual
    tokens[sp, pl.ds(own_row, rows), :width] = scaled_norm(residual.astype(f32), gain_ref[...].reshape(1, width)).astype(bf16)

    def block_of(group, slot):
        return tokens.at[group, pl.ds(pl.multiple_of(slot * rows, rows), rows), :]

    own_block = block_of(sp, 2 * c + y)
    block_copy = remote(own_block, own_block, y_sem.at[0], tok_recv.at[sp, 2 * c + y], at(sp, opposite))

    def forward(way, group, yy):
        device = (
            at(lax.rem(sp + 2, sp_count), tp),
            at(lax.rem(sp + sp_count - 2, sp_count), tp),
            at(across, tp),
            at(sp, sibling),
        )[way]
        block = block_of(group, 2 * c + yy)
        return remote(block, block, tok_send.at[way, group, yy], tok_recv.at[group, 2 * c + yy], device)

    def arrival(group, slot):
        block = block_of(group, slot)
        return remote(block, block, y_sem.at[0], tok_recv.at[group, slot], at(sp, sibling))

    def share(way, group):
        whose = tp if way < 2 else opposite
        block = hidden.at[group, whose]
        return remote(
            block, block, hid_send.at[way, group], hid_recv.at[group, whose], at(sp, sibling if way else opposite)
        )

    def shared(group, whose):
        block = hidden.at[group, whose]
        return remote(block, block, hid_send.at[0, group], hid_recv.at[group, whose], at(sp, sibling))

    near_first = [sorted(range(heights), key=lambda other: abs(other - i)) for i in range(heights)]
    home_order = [
        sorted(
            range(heights),
            key=lambda other: (other == i, heights - 1 - i if other < i else i, abs(other - i)),
        )
        for i in range(heights)
    ]

    def group_at(tick):
        height = table_pick(near_first, z, lax.div(tick, 2))
        own_x = lax.rem(tick, 2) == 0
        return height, 2 * height + jnp.where(own_x, x, 1 - x)

    def half_of(part_number):
        return pl.ds(part_number * half, half)

    def over_x(height, h):
        return remote(
            part.at[2 * height + 1 - x, half_of(h), :],
            x_in.at[height, half_of(h), :],
            x_send.at[height, h],
            x_recv.at[height, h],
            at(across, tp),
        )

    def homeward(height, down_side, h):
        device = at(lax.rem(sp + (sp_count - 2, 2)[down_side], sp_count), tp)
        return remote(
            part.at[2 * height + x, half_of(h), :],
            chain_in.at[down_side, height, half_of(h), :],
            chain_send.at[height, h],
            chain_recv.at[down_side, height, h],
            device,
        )

    last = heights - 1

    def own_side(step):
        height = table_pick(near_first, z, lax.div(step, 2))
        return height, jnp.where(lax.rem(step, 2) == 0, y, 1 - y)

    def take_own(height, yy):
        group = 2 * height + x
        arrival(group, 2 * c + yy).wait_recv()

        @pl.when((height <= z) & (z < last))
        def _():
            forward(0, group, yy).start()

        @pl.when((height >= z) & (z > 0))
        def _():
            forward(1, group, yy).start()

        forward(3, group, yy).start()

    def send_across(step):
        height, yy = own_side(step)
        forward(2, 2 * height + x, yy).start()

    def take_across(step):
        height, yy = own_side(step)
        group = 2 * height + 1 - x
        arrival(group, 2 * c + yy).wait_recv()
        forward(3, group, yy).start()

    def gated_units(tick):
        _, group = group_at(tick)
        for yy in range(2):
            arrival(group, 2 * (1 - c) + yy).wait_recv()
        inputs = tokens[group, :, :width]
        tile = min(256, units)
        for start in range(0, units, tile):
            gate_pre = jnp.dot(inputs, gate_w[:, start : start + tile], preferred_element_type=f32)
            up_pre = jnp.dot(inputs, up_w[:, start : start + tile], preferred_element_type=f32)
            hidden[group, tp, :, start : start + tile] = clamped_units(gate_pre, up_pre).astype(bf16)
        share(0, group).start()
        share(1, group).start()

    def relay_units(tick):
        _, group = group_at(tick)
        shared(group, opposite).wait_recv()
        share(2, group).start()

    def project_down(tick):
        height, group = group_at(tick)
        shared(group, sibling).wait_recv()
        shared(group, 3 - tp).wait_recv()
        total = jnp.dot(hidden[group, 0], down_w[:units, :], preferred_element_type=f32)
        for k in range(1, 4):
            total = total + jnp.dot(
                hidden[group, k], down_w[k * units : (k + 1) * units, :], preferred_element_type=f32
            )
        lanes = lax.broadcasted_iota(jnp.int32, (seq, LANES), 1)
        mine = (lanes == sp) | (lanes == sp + sp_count)
        scale = jnp.sum(jnp.where(mine, tokens[group, :, width:].astype(f32), 0.0), axis=1, keepdims=True)
        part[group] = (total.astype(bf16).astype(f32) * scale).astype(bf16)

        @pl.when((lax.rem(tick, 2) == 1) & (tick > 1))
        def _():
            for h in range(2):
                over_x(height, h).start()

    block_copy.start()
    for way, there in ((0, z < last), (1, z > 0)):

        @pl.when(there)
        def _():
            forward(way, sp, y).start()

    forward(2, sp, y).start()
    forward(3, sp, y).start()
    take_own(z, 1 - y)
    send_across(jnp.int32(1))
    for load in loads[1:]:
        load.wait()

    def take_step(step, yy):
        distance = lax.div(step, 2) + 1

        @pl.when(z >= distance)
        def _():
            take_own(z - distance, yy)

        @pl.when(z + distance <= last)
        def _():
            take_own(z + distance, yy)

        send_across(step + 2)

    gated_units(jnp.int32(0))

    def round_body(j, carry):
        early, late = 2 * j, 2 * j + 1

        @pl.when(j < last)
        def _():
            take_step(early, y)

        take_across(early)

        @pl.when(j >= 1)
        def _():
            relay_units(early - 1)
            project_down(early - 2)

        @pl.when(j < last)
        def _():
            take_step(late, 1 - y)

        take_across(late)
        gated_units(late)

        @pl.when(j < last)
        def _():
            gated_units(late + 1)

        relay_units(early)

        @pl.when(j >= 1)
        def _():
            project_down(early - 1)

        return carry

    lax.fori_loop(0, heights, round_body, 0)

    def f32_half(ref, index, h):
        return ref[index, half_of(h), :].astype(f32)

    def go_home(item):
        height = table_pick(home_order, z, item)
        group = 2 * height + x
        from_above = (height < z) & (z < last)
        from_below = (height > z) & (z > 0)
        for h in range(2):
            over_x(height, h).wait_recv()

            @pl.when(jnp.logical_not(from_above | from_below))
            def _():
                part[group, half_of(h), :] = (f32_half(part, group, h) + f32_half(x_in, height, h)).astype(bf16)

            for down_side, comes in enumerate((from_above, from_below)):

                @pl.when(comes)
                def _():
                    homeward(height, down_side, h).wait_recv()
                    total = f32_half(part, group, h) + f32_half(x_in, height, h)
                    total = total + chain_in[down_side, height, half_of(h), :].astype(f32)
                    part[group, half_of(h), :] = total.astype(bf16)

            @pl.when(height < z)
            def _():
                homeward(height, 0, h).start()

            @pl.when(height > z)
            def _():
                homeward(height, 1, h).start()

    at_end = (z == 0) | (z == last)
    early_items = min(2, last)

    def go_early(item):
        @pl.when(at_end)
        def _():
            go_home(jnp.int32(item))

    go_early(0)
    relay_units(sp_count - 1)
    project_down(sp_count - 2)
    if early_items > 1:
        go_early(1)
    project_down(sp_count - 1)
    for h in range(2):
        over_x(z, h).start()

    def home_body(item, carry):
        @pl.when(jnp.logical_not(at_end) | (item >= early_items))
        def _():
            go_home(item)

        return carry

    lax.fori_loop(0, last, home_body, 0)

    def hand_over(h, yy):
        return remote(
            final.at[pl.ds(h * half + yy * rows, rows), :],
            columns.at[tp],
            fin_send.at[2 * h + yy],
            fin_recv.at[tp],
            at(sp, 2 * yy + h),
        )

    for h in range(2):
        over_x(z, h).wait_recv()
        part[sp, half_of(h), :] = (f32_half(part, sp, h) + f32_half(x_in, z, h)).astype(bf16)
        for down_side, comes in enumerate((z < last, z > 0)):

            @pl.when(comes)
            def _():
                homeward(z, down_side, h).wait_recv()
                part[sp, half_of(h), :] = (
                    f32_half(part, sp, h) + chain_in[down_side, z, half_of(h), :].astype(f32)
                ).astype(bf16)

        final[half_of(h), :] = part[sp, half_of(h), :]
        for yy in range(2):

            @pl.when(tp != 2 * yy + h)
            def _():
                hand_over(h, yy).start()

    columns[tp] = final[pl.ds(own_row, rows), :]
    for step in (1, 2, 3):
        whose = lax.rem(tp + step, 4)
        remote(
            final.at[pl.ds(0, rows), :], columns.at[whose], fin_send.at[0], fin_recv.at[whose], at(sp, sibling)
        ).wait_recv()
    combined = jnp.concatenate([columns[k] for k in range(4)], 1).astype(f32)
    result_ref[...] = (
        resid[...].astype(f32) + scaled_norm(combined, post_gain_ref[...].reshape(1, width))
    ).astype(bf16)

    block_copy.wait_send()
    for h in range(2):
        for yy in range(2):

            @pl.when(tp != 2 * yy + h)
            def _():
                hand_over(h, yy).wait_send()

    def drain(group, carry):
        height = lax.div(group, 2)

        for yy in range(2):

            @pl.when(lax.rem(group, 2) == x)
            def _():
                @pl.when((height <= z) & (z < last))
                def _():
                    forward(0, group, yy).wait_send()

                @pl.when((height >= z) & (z > 0))
                def _():
                    forward(1, group, yy).wait_send()

                forward(2, group, yy).wait_send()

            forward(3, group, yy).wait_send()
        for way in range(3):
            share(way, group).wait_send()

        @pl.when(lax.rem(group, 2) == 0)
        def _():
            for h in range(2):
                over_x(height, h).wait_send()

                @pl.when(height != z)
                def _():
                    homeward(height, 0, h).wait_send()

        return carry

    lax.fori_loop(0, sp_count, drain, 0)


def dense_layer(
    stream_in,
    pre_gate,
    value_in,
    post_gate,
    conv_taps,
    out_weight,
    route_ids,
    route_weight,
    ffn_gain,
    post_gain,
    gate_proj,
    up_proj,
    down_proj,
):
    sp_count = lax.axis_size("sp")
    rows, width = stream_in.shape
    seq, channels = pre_gate.shape
    units = gate_proj.shape[2]
    cols = down_proj.shape[2]
    bf16, f32 = jnp.bfloat16, jnp.float32
    dma = pltpu.SemaphoreType.DMA
    scratch = [
        pltpu.VMEM(out_weight.shape, bf16),
        pltpu.VMEM(gate_proj.shape[1:], bf16),
        pltpu.VMEM(up_proj.shape[1:], bf16),
        pltpu.VMEM(down_proj.shape[1:], bf16),
        pltpu.VMEM((16, channels), bf16),
        pltpu.VMEM((16, channels), bf16),
        pltpu.VMEM((seq + 8, channels), f32),
        pltpu.VMEM((seq, channels), bf16),
        pltpu.VMEM((2 * rows, width), bf16),
        pltpu.VMEM((2 * rows, width), bf16),
        pltpu.VMEM((2 * rows, width), f32),
        pltpu.VMEM((rows, width), bf16),
        pltpu.VMEM((rows, width), bf16),
        pltpu.VMEM((rows, width), bf16),
        pltpu.VMEM((sp_count, seq, width + LANES), bf16),
        pltpu.VMEM((sp_count, 4, seq, units), bf16),
        pltpu.VMEM((sp_count, seq, cols), bf16),
        pltpu.VMEM((2, sp_count // 2, seq, cols), bf16),
        pltpu.VMEM((sp_count // 2, seq, cols), bf16),
        pltpu.VMEM((seq, cols), bf16),
        pltpu.VMEM((4, rows, cols), bf16),
        dma((4,)),
        dma((2,)),
        dma((4,)),
        dma((1,)),
        dma((4, sp_count, 2)),
        dma((sp_count, 4)),
        dma((3, sp_count)),
        dma((sp_count, 4)),
        dma((sp_count // 2, 2)),
        dma((2, sp_count // 2, 2)),
        dma((sp_count // 2, 2)),
        dma((sp_count // 2, 2)),
        dma((4,)),
        dma((4,)),
    ]
    vmem = pl.BlockSpec(memory_space=pltpu.VMEM)
    anywhere = pl.BlockSpec(memory_space=pl.ANY)
    return pl.pallas_call(
        functools.partial(layer_kernel, sp_count),
        out_shape=jax.ShapeDtypeStruct((rows, width), bf16),
        in_specs=[vmem] * 9 + [anywhere] * 4,
        out_specs=vmem,
        scratch_shapes=scratch,
        compiler_params=pltpu.CompilerParams(
            collective_id=0, has_side_effects=True, vmem_limit_bytes=58 * 1024 * 1024
        ),
    )(
        stream_in,
        pre_gate,
        value_in,
        post_gate,
        conv_taps,
        route_ids.T,
        route_weight.T,
        ffn_gain,
        post_gain,
        out_weight,
        gate_proj,
        up_proj,
        down_proj,
    )


def local(
    stream_in,
    pre_gate,
    value_in,
    post_gate,
    conv_taps,
    out_weight,
    route_ids,
    route_weight,
    ffn_gain,
    post_gain,
    gate_proj,
    up_proj,
    down_proj,
):
    sp_count = lax.axis_size("sp")
    tp_count = lax.axis_size("tp")
    seq_rows = pre_gate.shape[0]
    own_rows = seq_rows // tp_count
    top_count = route_ids.shape[1]
    slots_each = 2 * own_rows * top_count // sp_count
    if tp_count == 4 and sp_count % 2 == 0 and slots_each >= own_rows:
        return dense_layer(
            stream_in, pre_gate, value_in, post_gate, conv_taps, out_weight, route_ids, route_weight,
            ffn_gain, post_gain, gate_proj, up_proj, down_proj,
        )
    tap_count = conv_taps.shape[0]
    gated_input = (pre_gate.astype(jnp.float32) * value_in.astype(jnp.float32)).astype(jnp.bfloat16)
    rim_rows = passed_along(gated_input[seq_rows - tap_count + 1 :], "sp", 1)
    padded = jnp.concatenate([rim_rows, gated_input], 0).astype(jnp.float32)
    convolved = jnp.zeros(gated_input.shape, jnp.float32)
    for tap_index in range(tap_count):
        convolved = (
            convolved
            + conv_taps[tap_index].astype(jnp.float32)[None, :]
            * padded[tap_index : tap_index + seq_rows]
        )
    mixer_out = (post_gate.astype(jnp.float32) * convolved).astype(jnp.bfloat16)
    weight_rows = mixer_out
    projected = lax.psum_scatter(
        jnp.dot(weight_rows, out_weight, preferred_element_type=jnp.float32),
        "tp",
        scatter_dimension=0,
        tiled=True,
    )
    residual = (stream_in.astype(jnp.float32) + projected).astype(jnp.bfloat16)
    normed = scaled_norm(residual.astype(jnp.float32), ffn_gain).astype(jnp.bfloat16)
    slot_rank = block_ranks(route_ids, sp_count, own_rows)
    block_of = (jnp.arange(seq_rows, dtype=jnp.int32) // own_rows)[:, None]
    tp_index = lax.axis_index("tp")
    own_ids = lax.dynamic_slice_in_dim(route_ids, tp_index * own_rows, own_rows, 0)
    own_rank = lax.dynamic_slice_in_dim(slot_rank, tp_index * own_rows, own_rows, 0)
    own_slot = own_ids * slots_each + own_rank
    picker = slot_picker(own_slot, sp_count * slots_each)
    outgoing = jnp.dot(picker, normed, preferred_element_type=jnp.float32).astype(jnp.bfloat16)
    arrived = lax.all_to_all(outgoing, "sp", split_axis=0, concat_axis=0, tiled=True)
    portion = lax.all_gather(arrived, "tp", axis=0, tiled=True)
    gate_pre = jnp.dot(portion, gate_proj[0], preferred_element_type=jnp.float32)
    up_pre = jnp.dot(portion, up_proj[0], preferred_element_type=jnp.float32)
    hidden = clamped_units(gate_pre, up_pre).astype(jnp.bfloat16)
    weight_rows = down_proj[0]
    column_out = jnp.dot(
        lax.all_gather(hidden, "tp", axis=1, tiled=True),
        weight_rows,
        preferred_element_type=jnp.float32,
    ).astype(jnp.bfloat16)
    column_width = column_out.shape[1]
    returned = lax.all_to_all(
        column_out.reshape(tp_count, sp_count, slots_each, column_width),
        "sp",
        split_axis=1,
        concat_axis=1,
        tiled=True,
    )
    home_index = (block_of * sp_count + route_ids) * slots_each + slot_rank
    gathered_out = jnp.take(returned.reshape(-1, column_width), home_index.reshape(-1), axis=0)
    gathered_out = gathered_out.astype(jnp.float32).reshape(seq_rows, top_count, column_width)
    combined_cols = jnp.sum(gathered_out * route_weight[:, :, None], axis=1).astype(jnp.bfloat16)
    combined = lax.all_to_all(combined_cols, "tp", split_axis=0, concat_axis=1, tiled=True)
    layer_out = residual.astype(jnp.float32) + scaled_norm(combined.astype(jnp.float32), post_gain)
    return layer_out.astype(jnp.bfloat16)


def solution(mesh):
    placed = (
        P(("sp", "tp"), None),
        P("sp", "tp"),
        P("sp", "tp"),
        P("sp", "tp"),
        P(None, "tp"),
        P("tp", None),
        P("sp", None),
        P("sp", None),
        P(),
        P(),
        P("sp", None, "tp"),
        P("sp", None, "tp"),
        P("sp", None, "tp"),
    )
    return jax.shard_map(
        local, mesh=mesh, in_specs=placed, out_specs=P(("sp", "tp"), None), check_vma=False
    )
```
